32 devices in a mesh: fs: 8 (over z, x), tp: 4 (over y, core).
Axes of the slice: x: 2, y: 2, z: 4, core: 2. Of those that a mesh axis runs over, the one named last changes fastest.
Arguments:
- saved_input: bfloat16 [24576, 2048], P('fs'), may hold values from -6 to 6
- proj_cot: bfloat16 [3, 24576, 2048], P(None, 'fs', 'tp'), may hold values from -0.0390625 to 0.0390625
- log_cache: float32 [16, 24576], P(None, 'fs'), as said below
- cache_cot: float32 [16, 24576], P(None, 'fs'), may hold values from -0.0390625 to 0.0390625
- proj_master: float32 [3, 2048, 2048], P(None, 'fs', 'tp'), may hold values from -0.125 to 0.125
- factors: bfloat16 [3, 2048, 256], P(None, 'fs'), may hold values from -0.125 to 0.125
- first_moment: float32 [3, 256, 2048], P(None, None, 'tp'), may hold values from -6 to 6
- second_moment: float32 [3, 256, 2048], P(None, None, 'tp'), may hold values from 0.01 to 10
- gate_master: float32 [16, 2048], replicated, may hold values from -0.125 to 0.125
- gate_first: float32 [16, 2048], replicated, may hold values from -6 to 6
- gate_second: float32 [16, 2048], replicated, may hold values from 0.1 to 3
Outputs:
- proj_step: float32 [3, 2048, 2048], P(None, 'fs', 'tp')
- proj_new: float32 [3, 2048, 2048], P(None, 'fs', 'tp')
- proj_copy: bfloat16 [3, 2048, 2048], P(None, None, 'tp')
- first_new: float32 [3, 256, 2048], P(None, None, 'tp')
- second_new: float32 [3, 256, 2048], P(None, None, 'tp')
- gate_new: float32 [16, 2048], replicated
- gate_copy: bfloat16 [16, 2048], replicated
- gate_first_new: float32 [16, 2048], replicated
- gate_second_new: float32 [16, 2048], replicated
The draws below stay inside these ranges and needn't reach their ends.
Inputs may be any that keep to these rules, and one draw needn't show every extreme that they name: `log_cache`: each head's values never rise along positions.
All inputs are finite; a program needn't handle non-finite values.
Results may differ from the reference program's by a relative error of at most 0.0004.
Values may be sent and summed in bfloat16 or wider, within the bound.
A program may use at most 128 MiB of HBM per device.

```python
import math
import jax
import jax.numpy as jnp
from jax import lax

D = 2048
ATTENTION_HEADS = 16
RANK = 256
ROLES = 3
TOK_DEV = 3072
W = 2048
SEQUENCE_TOKENS = 24576


def draw_log_cache(key, part):
    keys = jax.random.split(key, 7)
    order = jax.random.permutation(keys[0], ATTENTION_HEADS)
    slow_decay = order < ATTENTION_HEADS // 2
    total = jnp.exp(jax.random.uniform(keys[1], (ATTENTION_HEADS, 1), jnp.float32, math.log(0.3), math.log(1.0)))
    fast_rate = jnp.exp(jax.random.uniform(keys[2], (ATTENTION_HEADS, 1), jnp.float32, math.log(0.01), math.log(1.0 / 30.0)))
    learning_rate = jnp.where(slow_decay[:, None], total / SEQUENCE_TOKENS, fast_rate)
    blocks = SEQUENCE_TOKENS // TOK_DEV
    block_multiplier = jnp.exp(jax.random.uniform(keys[3], (ATTENTION_HEADS, blocks), jnp.float32, math.log(0.5), math.log(2.0)))
    block_multiplier = jnp.repeat(block_multiplier, TOK_DEV, axis=1)
    coarse_estimate = jnp.exp(jax.random.uniform(keys[4], (ATTENTION_HEADS, SEQUENCE_TOKENS), jnp.float32, -0.7, 0.7))
    chosen_locations = jax.random.randint(keys[5], (ATTENTION_HEADS, 3), 0, SEQUENCE_TOKENS)
    layer_depth = jax.random.uniform(keys[6], (ATTENTION_HEADS, 3), jnp.float32, 0.22, 0.5)
    target_positions = jnp.arange(SEQUENCE_TOKENS)
    sudden_spike = jnp.zeros((ATTENTION_HEADS, SEQUENCE_TOKENS), jnp.float32)
    for position_index in range(3):
        sudden_spike = sudden_spike + jnp.where(target_positions[None, :] == chosen_locations[:, position_index:position_index + 1], layer_depth[:, position_index:position_index + 1], 0.0)
    gate_logarithm = -(learning_rate * block_multiplier * coarse_estimate) - sudden_spike * slow_decay[:, None].astype(jnp.float32)
    return jnp.cumsum(gate_logarithm, axis=1)


def draw_second_moment(key, part):
    lower, upper, fall = (1.0, 10.0, 10.0)
    base = jnp.exp(jax.random.uniform(key, (ROLES, RANK, W), jnp.float32, math.log(lower), math.log(upper)))
    column = jnp.arange(W, dtype=jnp.float32) / W
    return base * jnp.power(fall, -column)[None, None, :]


def block_levels(rng, dims, shards, smallest, largest):
    level, own = 1.0, jax.random.fold_in(rng, 6)
    for position, parts in shards:
        draws = jnp.exp(jax.random.uniform(jax.random.fold_in(own, position), (parts,), jnp.float32, smallest / len(shards), largest / len(shards)))
        level = level * jnp.repeat(draws, dims[position] // parts).reshape([-1 if axis == position else 1 for axis in range(len(dims))])
    return level


def scatter_about(stream_key, extent, spread, reach, cuts=(), held_as=jnp.bfloat16):
    factor_of = block_levels(stream_key, extent, cuts, -0.22, 0.18) if cuts else 1.0
    drawn = jax.random.normal(stream_key, extent, jnp.float32) * spread * factor_of
    return jnp.minimum(jnp.maximum(drawn, -reach), reach).astype(held_as)


def setup_inputs(seed: int = 0) -> dict:
    splits = jax.random.split(jax.random.key(seed), 12)
    saved_input = scatter_about(splits[0], (SEQUENCE_TOKENS, D), 1.0, 6.0, ((0, 8),))
    proj_cot = scatter_about(splits[1], (ROLES, SEQUENCE_TOKENS, W), SEQUENCE_TOKENS ** -0.5, 0.0390625, ((1, 8), (2, 4)))
    log_cache = draw_log_cache(jax.random.fold_in(splits[11], 71), 0)
    cache_cot = scatter_about(splits[3], (ATTENTION_HEADS, SEQUENCE_TOKENS), SEQUENCE_TOKENS ** -0.5, 0.0390625, ((1, 8),), jnp.float32)
    proj_master = scatter_about(splits[4], (ROLES, D, W), D ** -0.5, 0.125, ((1, 8), (2, 4)), jnp.float32)
    factors = scatter_about(splits[5], (ROLES, D, RANK), D ** -0.5, 0.125, ((1, 8),))
    first_moment = scatter_about(splits[6], (ROLES, RANK, W), 1.0, 6.0, ((2, 4),), jnp.float32)
    second_moment = draw_second_moment(jax.random.fold_in(splits[11], 71), 0)
    gate_master = scatter_about(splits[8], (ATTENTION_HEADS, D), D ** -0.5, 0.125, (), jnp.float32)
    gate_first = scatter_about(splits[9], (ATTENTION_HEADS, D), 1.0, 6.0, (), jnp.float32)
    gate_second = jnp.clip(jnp.exp(jax.random.uniform(splits[10], (ATTENTION_HEADS, D), jnp.float32, math.log(0.1), math.log(3.0))), 0.1, 3.0)
    return {"saved_input": saved_input, "proj_cot": proj_cot, "log_cache": log_cache, "cache_cot": cache_cot, "proj_master": proj_master, "factors": factors, "first_moment": first_moment, "second_moment": second_moment, "gate_master": gate_master, "gate_first": gate_first, "gate_second": gate_second}


BETA_ONE = 0.8
BETA_TWO = 0.9
LEARN = 0.001

def reference(saved_input, proj_cot, log_cache, cache_cot, proj_master, factors, first_moment, second_moment, gate_master, gate_first, gate_second):
    lows = []
    for role in range(ROLES):
        grad = jnp.dot(saved_input.T, proj_cot[role], preferred_element_type=jnp.float32)
        lows.append(jnp.dot(factors[role].astype(jnp.float32).T, grad, precision=lax.Precision.HIGHEST))
    low = jnp.stack(lows)
    first_new = BETA_ONE * first_moment + (1.0 - BETA_ONE) * low
    second_new = BETA_TWO * second_moment + (1.0 - BETA_TWO) * low * low
    direction = first_new / jnp.sqrt(second_new)
    scale = lax.rsqrt(jnp.mean(direction * direction) + 1e-06)
    product = jnp.einsum('rdk,rkw->rdw', factors.astype(jnp.float32), direction, precision=lax.Precision.HIGHEST)
    proj_step = scale * product
    proj_new = proj_master - LEARN * proj_step
    proj_copy = proj_new.astype(jnp.bfloat16)
    previous = jnp.concatenate([jnp.zeros((ATTENTION_HEADS, 1), jnp.float32), log_cache[:, :-1]], axis=1)
    gate_logarithm = log_cache - previous
    later = jnp.flip(jnp.cumsum(jnp.flip(cache_cot, 1), axis=1), 1)
    gate_cot = (later * -jnp.expm1(gate_logarithm)).astype(jnp.bfloat16)
    gate_grad = jnp.dot(gate_cot, saved_input, preferred_element_type=jnp.float32)
    gate_first_new = BETA_ONE * gate_first + (1.0 - BETA_ONE) * gate_grad
    gate_second_new = BETA_TWO * gate_second + (1.0 - BETA_TWO) * gate_grad * gate_grad
    gate_new = gate_master - LEARN * gate_first_new / jnp.sqrt(gate_second_new)
    gate_copy = gate_new.astype(jnp.bfloat16)
    return (proj_step, proj_new, proj_copy, first_new, second_new, gate_new, gate_copy, gate_first_new, gate_second_new)
```

```python
import functools

import jax
import jax.numpy as jnp
from jax import lax
from jax.experimental import pallas as pl
from jax.experimental.pallas import tpu as pltpu
from jax.sharding import PartitionSpec as P

BETA_ONE = 0.8
BETA_TWO = 0.9
LEARN = 0.001
LANES = 128
HIGH = lax.Precision.HIGHEST
MESH = pl.DeviceIdType.MESH


def ring_order(count):
    wide = max(count // 4, 1)
    tall = count // wide
    if wide == 1 or tall % 2:
        return list(range(count))
    path = [0]
    for row in range(tall):
        across = range(1, wide)
        for column in across if row % 2 == 0 else reversed(across):
            path.append(row * wide + column)
    path += [row * wide for row in range(tall - 1, 0, -1)]
    return path


def pick(table, index):
    found = jnp.int32(table[0])
    for position, value in enumerate(table):
        if position:
            found = jnp.where(index == position, jnp.int32(value), found)
    return found


class Ring:
    def __init__(self, count):
        self.count = count
        self.order = ring_order(count)
        places = [0] * count
        for position, member in enumerate(self.order):
            places[member] = position
        self.me = lax.axis_index("fs")
        self.place = pick(places, self.me)

    def ahead(self, way, by):
        step = by if way == 0 else -by
        return pick(self.order, lax.rem(self.place + step + 2 * self.count, self.count))

    def hops(self, way, half):
        return self.count // 2 if way == half else self.count - 1 - self.count // 2

    def greet(self, partner=None):
        barrier = pltpu.get_barrier_semaphore()
        for way in range(2):
            pl.semaphore_signal(
                barrier, inc=1, device_id={"fs": self.ahead(way, 1)}, device_id_type=MESH
            )
        if partner is not None:
            pl.semaphore_signal(barrier, inc=1, device_id={"tp": partner}, device_id_type=MESH)
        pl.semaphore_wait(barrier, 2 if partner is None else 3)


def remote(source, target, send, receive, device):
    return pltpu.make_async_remote_copy(
        src_ref=source,
        dst_ref=target,
        send_sem=send,
        recv_sem=receive,
        device_id=device,
        device_id_type=MESH,
    )


def spread(ring, pieces, send, receive):
    most = ring.count // 2
    sent = []
    for hop in range(most):
        for number, (half, first, at) in enumerate(pieces):
            for way in range(2):
                if hop >= ring.hops(way, half):
                    continue
                origin = ring.ahead(way, -hop)
                place = at(origin)
                if hop:
                    remote(place, place, send.at[way, number, hop - 1], receive.at[way, number, hop - 1], {"fs": ring.ahead(way, 1)}).wait_recv()
                copy = remote(
                    first if hop == 0 else place,
                    place,
                    send.at[way, number, hop],
                    receive.at[way, number, hop],
                    {"fs": ring.ahead(way, 1)},
                )
                copy.start()
                sent.append(copy)
    for number, (half, first, at) in enumerate(pieces):
        for way in range(2):
            last = ring.hops(way, half)
            place = at(ring.ahead(way, -last))
            remote(place, place, send.at[way, number, last - 1], receive.at[way, number, last - 1], {"fs": ring.ahead(way, 1)}).wait_recv()
    for copy in sent:
        copy.wait_send()


def copy_gather(count, block, out, send, receive):
    ring = Ring(count)
    ring.greet()
    roles, rows, width = block.shape
    part = rows // 2

    def at(role, half, origin):
        return out.at[role, pl.ds(pl.multiple_of(origin * rows + half * part, part), part)]

    pieces = [
        (half, block.at[role, pl.ds(half * part, part)], functools.partial(at, role, half))
        for role in range(roles)
        for half in range(2)
    ]
    for role in range(roles):
        out[role, pl.ds(pl.multiple_of(ring.me * rows, rows), rows)] = block[role]
    spread(ring, pieces, send, receive)


def gather_copies(block, count):
    roles, rows, width = block.shape
    slots = (2, 2 * roles, count // 2)
    return pl.pallas_call(
        functools.partial(copy_gather, count),
        out_shape=jax.ShapeDtypeStruct((roles, rows * count, width), block.dtype),
        in_specs=[pl.BlockSpec(memory_space=pltpu.VMEM)],
        out_specs=pl.BlockSpec(memory_space=pltpu.VMEM),
        scratch_shapes=[pltpu.SemaphoreType.DMA(slots), pltpu.SemaphoreType.DMA(slots)],
        compiler_params=pltpu.CompilerParams(collective_id=2, has_side_effects=True),
    )(block)


def factor_gather(count, block, stats, out, all_stats, send, receive, give, take):
    ring = Ring(count)
    tp = lax.axis_index("tp")
    core = lax.rem(tp, 2)
    partner = tp + 1 - 2 * core
    ring.greet(partner)
    roles, rows, rank = block.shape
    part = rows // 2
    half_rank = rank // 2
    mine = pl.ds(pl.multiple_of(core * half_rank, half_rank), half_rank)

    def at(half, origin):
        return out.at[:, pl.ds(pl.multiple_of(origin * rows + half * part, part), part), mine]

    def stats_at(origin):
        return all_stats.at[origin]

    pieces = [(0, stats, stats_at)] + [
        (half, block.at[:, pl.ds(half * part, part), mine], functools.partial(at, half))
        for half in range(2)
    ]
    all_stats[ring.me] = stats[...]
    out[:, pl.ds(pl.multiple_of(ring.me * rows, rows), rows), :] = block[...]
    most = count // 2
    sent = []

    def arrived(way, number, hop):
        place = pieces[number][2](ring.ahead(way, -hop))
        remote(place, place, send.at[way, number, hop - 1], receive.at[way, number, hop - 1], {"fs": ring.ahead(way, 1)}).wait_recv()
        return place

    def share(way, number, hop, place):
        copy = remote(place, place, give.at[way, number - 1, hop - 1], take.at[way, number - 1, hop - 1], {"tp": partner})
        copy.start()
        sent.append(copy)

    for hop in range(most + 1):
        for number, (half, first, at_origin) in enumerate(pieces):
            for way in range(2):
                hops = ring.hops(way, half)
                if hop > hops:
                    continue
                source = first
                if hop:
                    source = arrived(way, number, hop)
                if hop < hops:
                    copy = remote(
                        source,
                        at_origin(ring.ahead(way, -hop)),
                        send.at[way, number, hop],
                        receive.at[way, number, hop],
                        {"fs": ring.ahead(way, 1)},
                    )
                    copy.start()
                    sent.append(copy)
                if hop and number:
                    share(way, number, hop, source)
    theirs = pl.ds(pl.multiple_of((1 - core) * half_rank, half_rank), half_rank)
    for number, (half, first, at_origin) in enumerate(pieces):
        if not number:
            continue
        for way in range(2):
            for hop in range(1, ring.hops(way, half) + 1):
                origin = ring.ahead(way, -hop)
                place = out.at[:, pl.ds(pl.multiple_of(origin * rows + half * part, part), part), theirs]
                remote(place, place, give.at[way, number - 1, hop - 1], take.at[way, number - 1, hop - 1], {"tp": partner}).wait_recv()
    for copy in sent:
        copy.wait_send()


def gather_factors(block, stats, count):
    roles, rows, rank = block.shape
    slots = (2, 3, count // 2)
    shares = (2, 2, count // 2)
    vmem = pl.BlockSpec(memory_space=pltpu.VMEM)
    return pl.pallas_call(
        functools.partial(factor_gather, count),
        out_shape=(
            jax.ShapeDtypeStruct((roles, rows * count, rank), block.dtype),
            jax.ShapeDtypeStruct((count,) + stats.shape, stats.dtype),
        ),
        in_specs=[vmem, vmem],
        out_specs=(vmem, vmem),
        scratch_shapes=[
            pltpu.SemaphoreType.DMA(slots),
            pltpu.SemaphoreType.DMA(slots),
            pltpu.SemaphoreType.DMA(shares),
            pltpu.SemaphoreType.DMA(shares),
        ],
        compiler_params=pltpu.CompilerParams(collective_id=0, has_side_effects=True),
    )(block, stats)


def sum_over_ring(count, terms, out, came, sums, send, receive, send_more, receive_more):
    ring = Ring(count)
    ring.greet()
    rows = terms.shape[0] // count
    half_width = terms.shape[1] // 2
    most = count // 2

    def own(member, half):
        return terms.at[pl.ds(pl.multiple_of(member * rows, rows), rows), pl.ds(half * half_width, half_width)]

    sent = []

    def wait(way, half, hop):
        slot = came.at[way, half, hop]
        remote(slot, slot, send.at[way, half, hop], receive.at[way, half, hop], {"fs": ring.ahead(way, 1)}).wait_recv()

    for hop in range(most):
        for late in range(2):
            for way in range(2):
                half = way if late == 0 else 1 - way
                hops = ring.hops(way, half)
                if hop >= hops:
                    continue
                term = own(ring.ahead(way, hops - hop), half)
                if hop:
                    wait(way, half, hop - 1)
                    sums[way, half, hop] = came[way, half, hop - 1] + term[...]
                    term = sums.at[way, half, hop]
                copy = remote(term, came.at[way, half, hop], send.at[way, half, hop], receive.at[way, half, hop], {"fs": ring.ahead(way, 1)})
                copy.start()
                sent.append(copy)
    mine = pl.ds(pl.multiple_of(ring.me * rows, rows), rows)
    for half in range(2):
        total = own(ring.me, half)[...]
        for way in range(2):
            last = ring.hops(way, half) - 1
            wait(way, half, last)
            total = total + came[way, half, last]
        out[mine, pl.ds(half * half_width, half_width)] = total

    def at(half, origin):
        return out.at[pl.ds(pl.multiple_of(origin * rows, rows), rows), pl.ds(half * half_width, half_width)]

    pieces = [(half, at(half, ring.me), functools.partial(at, half)) for half in range(2)]
    spread(ring, pieces, send_more, receive_more)
    for copy in sent:
        copy.wait_send()


def ring_sum(terms, count):
    rows, width = terms.shape
    slots = (2, 2, count // 2)
    vmem = pl.BlockSpec(memory_space=pltpu.VMEM)
    held = pltpu.VMEM(slots + (rows // count, width // 2), jnp.float32)
    return pl.pallas_call(
        functools.partial(sum_over_ring, count),
        out_shape=jax.ShapeDtypeStruct(terms.shape, terms.dtype),
        in_specs=[vmem],
        out_specs=vmem,
        scratch_shapes=[held, held] + [pltpu.SemaphoreType.DMA(slots)] * 4,
        compiler_params=pltpu.CompilerParams(collective_id=1, has_side_effects=True),
    )(terms)


def sums_from(values):
    heads, length = values.shape
    blocks = values.reshape(heads, length // LANES, LANES)
    place = jnp.arange(LANES)
    inside = jnp.einsum(
        "hbt,ts->hbs", blocks, (place[:, None] >= place[None, :]).astype(jnp.float32), precision=HIGH
    )
    which = jnp.arange(length // LANES)
    after = jnp.einsum(
        "hb,bc->hc",
        inside[:, :, 0],
        (which[:, None] > which[None, :]).astype(jnp.float32),
        precision=HIGH,
    )
    return (inside + after[:, :, None]).reshape(heads, length)


def local(
    saved_input,
    proj_cot,
    log_cache,
    cache_cot,
    proj_master,
    factors,
    first_moment,
    second_moment,
    gate_master,
    gate_first,
    gate_second,
):
    heads = log_cache.shape[0]
    count = lax.axis_size("fs")
    me = lax.axis_index("fs")
    totals = jnp.sum(cache_cot, axis=1, keepdims=True)
    edges = log_cache[:, -1:]
    stats = jnp.concatenate(
        [totals, edges, jnp.zeros((heads, LANES - 2), jnp.float32)], axis=1
    )
    all_factors, all_stats = gather_factors(factors, stats, count)
    members = jnp.arange(count)[:, None]
    carried = jnp.sum(jnp.where(members > me, all_stats[:, :, 0], 0.0), axis=0)
    edge = jnp.sum(jnp.where(members == me - 1, all_stats[:, :, 1], 0.0), axis=0)
    previous = jnp.concatenate([edge[:, None], log_cache[:, :-1]], axis=1)
    gate_logarithm = log_cache - previous
    later = sums_from(cache_cot) + carried[:, None]
    gate_cot = (later * -jnp.expm1(gate_logarithm)).astype(jnp.bfloat16)
    gate_part = jnp.dot(gate_cot, saved_input, preferred_element_type=jnp.float32)
    reduced = jnp.einsum(
        "td,rdk->rtk", saved_input, all_factors, preferred_element_type=jnp.float32
    )
    upper_half = lax.optimization_barrier(reduced.astype(jnp.bfloat16))
    lower_half = (reduced - upper_half.astype(jnp.float32)).astype(jnp.bfloat16)
    low_part = jnp.einsum("rtk,rtw->rkw", upper_half, proj_cot, preferred_element_type=jnp.float32)
    low_part = low_part + jnp.einsum(
        "rtk,rtw->rkw", lower_half, proj_cot, preferred_element_type=jnp.float32
    )
    roles, rank, width = low_part.shape
    flat_low = low_part.reshape(roles * rank, width)
    flat_gate = gate_part.reshape(-1, width)
    used = flat_low.shape[0] + flat_gate.shape[0]
    spare = -used % (8 * count)
    terms = jnp.concatenate([flat_low, flat_gate, jnp.zeros((spare, width), jnp.float32)])
    total = ring_sum(terms, count)
    low = total[: roles * rank].reshape(low_part.shape)
    gate_grad = total[roles * rank : used].reshape(gate_part.shape)
    first_new = BETA_ONE * first_moment + (1.0 - BETA_ONE) * low
    second_new = BETA_TWO * second_moment + (1.0 - BETA_TWO) * low * low
    direction = first_new / jnp.sqrt(second_new)
    squares = lax.psum(jnp.sum(direction * direction), "tp")
    entries = direction.shape[0] * direction.shape[1] * direction.shape[2] * lax.axis_size("tp")
    scale = lax.rsqrt(squares / entries + 1e-06)
    product = jnp.einsum(
        "rdk,rkw->rdw", factors.astype(jnp.float32), direction, precision=lax.Precision.HIGHEST
    )
    proj_step = scale * product
    proj_new = proj_master - LEARN * proj_step
    proj_copy = gather_copies(proj_new.astype(jnp.bfloat16), count)
    gate_first_new = BETA_ONE * gate_first + (1.0 - BETA_ONE) * gate_grad
    gate_second_new = BETA_TWO * gate_second + (1.0 - BETA_TWO) * gate_grad * gate_grad
    gate_new = gate_master - LEARN * gate_first_new / jnp.sqrt(gate_second_new)
    gate_copy = gate_new.astype(jnp.bfloat16)
    return (
        proj_step,
        proj_new,
        proj_copy,
        first_new,
        second_new,
        gate_new,
        gate_copy,
        gate_first_new,
        gate_second_new,
    )


def solution(mesh):
    placed = (
        P("fs", None),
        P(None, "fs", "tp"),
        P(None, "fs"),
        P(None, "fs"),
        P(None, "fs", "tp"),
        P(None, "fs", None),
        P(None, None, "tp"),
        P(None, None, "tp"),
        P(),
        P(),
        P(),
    )
    return jax.shard_map(
        local,
        mesh=mesh,
        in_specs=placed,
        out_specs=(
            P(None, "fs", "tp"),
            P(None, "fs", "tp"),
            P(None, None, "tp"),
            P(None, None, "tp"),
            P(None, None, "tp"),
            P(),
            P(),
            P(),
            P(),
        ),
        check_vma=False,
    )
```
